32 devices in a mesh: sp: 16 (over z, y, x), tp: 2 (over core).
Axes of the slice: x: 2, y: 2, z: 4, core: 2. Of those that a mesh axis runs over, the one named last changes fastest.
Arguments:
- tokens: bfloat16 [16384, 2048], P('sp', 'tp'), may hold values from -6 to 6
- norm_gain: float32 [2048], replicated, may hold values from 0.1 to 1.9
- w_query: bfloat16 [2048, 1024], P('sp', 'tp'), may hold values from -0.125 to 0.125
- w_key: bfloat16 [2048, 512], P('sp', 'tp'), may hold values from -0.125 to 0.125
- w_value: bfloat16 [2048, 512], P('sp', 'tp'), may hold values from -0.125 to 0.125
- w_glu_a: bfloat16 [2048, 1024], P('sp', 'tp'), may hold values from -0.125 to 0.125
- w_glu_b: bfloat16 [2048, 1024], P('sp', 'tp'), may hold values from -0.125 to 0.125
- q_gain: float32 [64], replicated, may hold values from 0.8 to 7
- k_gain: float32 [64], replicated, may hold values from 0.8 to 7
- sink_logit: float32 [16], P('tp'), may hold values from 1 to 4
- conv_taps: float32 [31, 1024], P(None, 'tp'), may hold values from -1 to 1
- chan_gain: float32 [1024], P('tp'), may hold values from 0.1 to 1.9
- chan_bias: float32 [1024], P('tp'), may hold values from -3 to 3
- w_attn_back: bfloat16 [2048, 1024], P('sp', 'tp'), may hold values from -0.1875 to 0.1875
- w_conv_back: bfloat16 [2048, 1024], P('sp', 'tp'), may hold values from -0.1875 to 0.1875
Outputs:
- mixed: bfloat16 [16384, 2048], P(('sp', 'tp'))
- log_weight: float32 [16, 16384], P('tp', 'sp')
The draws below stay inside these ranges and needn't reach their ends.
All inputs are finite; a program needn't handle non-finite values.
Results may differ from the reference program's by a relative error of at most 0.014.
The reference program's roundings to bfloat16 on the way count: a program that leaves them out, or rounds other values in their place, can miss the bound.
Values may be sent and summed in bfloat16 or wider, within the bound.
No kernel may reach another device: no remote copies, remote signals or barrier semaphores. Data moves between devices by JAX's collectives and lax.ppermute only.
A program may use at most 128 MiB of HBM per device.

```python
import jax
import jax.numpy as jnp
from jax import lax

D = 2048
HEAD = 64
Q_HEADS = 16
KV_HEADS = 8
CH = 1024
KW = 31
WINDOW = 128
TOKENS = 16384
N_TP = 2


def draw_q_gain(key, part):
    own_key = jax.random.fold_in(key, 11)
    return jax.random.uniform(own_key, (HEAD,), jnp.float32, 0.8, 1.2)


def draw_k_gain(key, part):
    own_key = jax.random.fold_in(key, 23)
    return jax.random.uniform(own_key, (HEAD,), jnp.float32, 0.8, 1.2)


def levels(rng, dims, split, least, high):
    gain = 1.0
    for dim, parts in split:
        draws = jax.random.uniform(jax.random.fold_in(jax.random.fold_in(rng, 6), dim), (parts,), jnp.float32, least / len(split), high / len(split))
        gain = gain * jnp.repeat(jnp.exp(draws), dims[dim] // parts).reshape((-1,) + (1,) * (len(dims) - 1 - dim))
    return gain


def normal_values(rng, extent, deviation, most, shards=(), held_as=jnp.bfloat16):
    drawn = deviation * jax.random.normal(rng, extent, jnp.float32)
    if shards:
        drawn = drawn * levels(rng, extent, shards, -0.22, 0.18)
    return jnp.clip(drawn, -most, most).astype(held_as)


def setup_inputs(seed: int = 0) -> dict:
    streams_of = jax.random.split(jax.random.key(seed), 16)
    return {
        "tokens": normal_values(streams_of[0], (TOKENS, D), 1.0, 6.0, ((0, 16), (1, 2))),
        "norm_gain": jnp.clip(1.0 + 0.18 * jax.random.normal(streams_of[1], (D,), jnp.float32), 0.1, 1.9),
        "w_query": normal_values(streams_of[2], (D, Q_HEADS * HEAD), D ** -0.5, 0.125, ((0, 16), (1, 2))),
        "w_key": normal_values(streams_of[3], (D, KV_HEADS * HEAD), D ** -0.5, 0.125, ((0, 16), (1, 2))),
        "w_value": normal_values(streams_of[4], (D, KV_HEADS * HEAD), D ** -0.5, 0.125, ((0, 16), (1, 2))),
        "w_glu_a": normal_values(streams_of[5], (D, CH), D ** -0.5, 0.125, ((0, 16), (1, 2))),
        "w_glu_b": normal_values(streams_of[6], (D, CH), D ** -0.5, 0.125, ((0, 16), (1, 2))),
        "q_gain": draw_q_gain(jax.random.fold_in(streams_of[15], 71), 0),
        "k_gain": draw_k_gain(jax.random.fold_in(streams_of[15], 71), 0),
        "sink_logit": jnp.clip(1.0 + 3.0 * jax.random.uniform(streams_of[9], (Q_HEADS,), jnp.float32) ** levels(streams_of[9], (Q_HEADS,), ((0, 2),), -0.2, 0.2), 1.0, 4.0),
        "conv_taps": normal_values(streams_of[10], (KW, CH), KW ** -0.5, 1.0, ((1, 2),), jnp.float32),
        "chan_gain": jnp.clip(1.0 + 0.18 * jax.random.normal(streams_of[11], (CH,), jnp.float32), 0.1, 1.9),
        "chan_bias": normal_values(streams_of[12], (CH,), 0.5, 3.0, ((0, 2),), jnp.float32),
        "w_attn_back": normal_values(streams_of[13], (D, Q_HEADS * HEAD), (Q_HEADS * HEAD) ** -0.5, 0.1875, ((0, 16), (1, 2))),
        "w_conv_back": normal_values(streams_of[14], (D, CH), CH ** -0.5, 0.1875, ((0, 16), (1, 2))),
    }


EPS = 1e-06

def row_norm(inputs, scale_vec):
    squares = lax.optimization_barrier(jnp.mean(inputs * inputs, axis=-1, keepdims=True))
    return inputs * lax.rsqrt(squares + EPS) * scale_vec

def reference(tokens, norm_gain, w_query, w_key, w_value, w_glu_a, w_glu_b, q_gain, k_gain, sink_logit, conv_taps, chan_gain, chan_bias, w_attn_back, w_conv_back):
    seq_total = tokens.shape[0]
    group_size = Q_HEADS // KV_HEADS
    normed = row_norm(tokens.astype(jnp.float32), norm_gain).astype(jnp.bfloat16)
    query_raw = jnp.dot(normed, w_query, preferred_element_type=jnp.float32)
    key_raw = jnp.dot(normed, w_key, preferred_element_type=jnp.float32)
    value_raw = jnp.dot(normed, w_value, preferred_element_type=jnp.float32)
    glu_a = jnp.dot(normed, w_glu_a, preferred_element_type=jnp.float32)
    glu_b = jnp.dot(normed, w_glu_b, preferred_element_type=jnp.float32)
    queries = row_norm(query_raw.reshape(seq_total, Q_HEADS, HEAD), q_gain).astype(jnp.bfloat16)
    key_rows = row_norm(key_raw.reshape(seq_total, KV_HEADS, HEAD), k_gain).astype(jnp.bfloat16)
    value_rows = value_raw.astype(jnp.bfloat16).reshape(seq_total, KV_HEADS, HEAD)
    gated_rows = (glu_a * jax.nn.sigmoid(glu_b)).astype(jnp.bfloat16)
    zero_keys = jnp.zeros((WINDOW, KV_HEADS, HEAD), jnp.bfloat16)
    keys_padded = jnp.concatenate([zero_keys, key_rows], 0)
    values_padded = jnp.concatenate([zero_keys, value_rows], 0)
    offsets = jnp.arange(WINDOW, dtype=jnp.int32)
    band_offsets = jnp.arange(2 * WINDOW, dtype=jnp.int32)
    distance = WINDOW + offsets[:, None] - band_offsets[None, :]
    allowed = (distance >= 0) & (distance < WINDOW)
    sink_table = sink_logit.reshape(KV_HEADS, group_size)[:, :, None, None]

    def one_block(block_index):
        block_start = (block_index * WINDOW).astype(jnp.int32)
        query_block = lax.dynamic_slice_in_dim(queries, block_start, WINDOW, 0).astype(jnp.float32)
        query_block = query_block.reshape(WINDOW, KV_HEADS, group_size, HEAD)
        key_band = lax.dynamic_slice_in_dim(keys_padded, block_start, 2 * WINDOW, 0).astype(jnp.float32)
        value_band = lax.dynamic_slice_in_dim(values_padded, block_start, 2 * WINDOW, 0).astype(jnp.float32)
        scores = jnp.einsum('qhgd,khd->hgqk', query_block, key_band) * HEAD ** (-0.5)
        visible = allowed & (block_start - WINDOW + band_offsets[None, :] >= 0)
        masked = jnp.where(visible, scores, -jnp.inf)
        largest = jnp.maximum(lax.optimization_barrier(jnp.max(masked, axis=-1, keepdims=True)), sink_table)
        weights = jnp.where(visible, jnp.exp(scores - largest), 0.0)
        weight_sum = lax.optimization_barrier(jnp.sum(weights, axis=-1, keepdims=True)) + jnp.exp(sink_table - largest)
        log_sum = (largest + jnp.log(weight_sum))[..., 0].reshape(Q_HEADS, WINDOW)
        probabilities = (weights / weight_sum).astype(jnp.bfloat16)
        mixed_rows = jnp.einsum('hgqk,khd->qhgd', probabilities.astype(jnp.float32), value_band)
        return (mixed_rows.astype(jnp.bfloat16).reshape(WINDOW, Q_HEADS * HEAD), log_sum)
    block_count = seq_total // WINDOW
    attended, log_sums = lax.map(one_block, jnp.arange(block_count, dtype=jnp.int32))
    attended = attended.reshape(seq_total, Q_HEADS * HEAD)
    log_weight = jnp.transpose(log_sums, (1, 0, 2)).reshape(Q_HEADS, seq_total)
    zero_rim = jnp.zeros((KW - 1, CH), jnp.float32)
    extended = jnp.concatenate([zero_rim, gated_rows.astype(jnp.float32)], 0)
    convolved = jnp.zeros((seq_total, CH), jnp.float32)
    for tap_index in range(KW):
        convolved = convolved + conv_taps[tap_index] * extended[tap_index:tap_index + seq_total]
    center = lax.optimization_barrier(jnp.mean(convolved, axis=-1, keepdims=True))
    spread = lax.optimization_barrier(jnp.mean(convolved * convolved, axis=-1, keepdims=True)) - center * center
    normal = (convolved - center) * lax.rsqrt(spread + EPS) * chan_gain + chan_bias
    conv_rows = jax.nn.silu(normal).astype(jnp.bfloat16)
    attn_cols = Q_HEADS * HEAD // N_TP
    conv_cols = CH // N_TP
    summed = jnp.zeros((seq_total, D), jnp.float32)
    for shard_index in range(N_TP):
        attn_lo = shard_index * attn_cols
        conv_lo = shard_index * conv_cols
        partial_sum = jnp.dot(attended[:, attn_lo:attn_lo + attn_cols], w_attn_back[:, attn_lo:attn_lo + attn_cols].T, preferred_element_type=jnp.float32)
        partial_sum = partial_sum + jnp.dot(conv_rows[:, conv_lo:conv_lo + conv_cols], w_conv_back[:, conv_lo:conv_lo + conv_cols].T, preferred_element_type=jnp.float32)
        rounded = lax.optimization_barrier(partial_sum.astype(jnp.bfloat16))
        summed = summed + rounded.astype(jnp.float32)
    return (summed.astype(jnp.bfloat16), log_weight)
```

```python
import jax
import jax.numpy as jnp
from jax import lax
from jax.sharding import PartitionSpec as P

HEAD = 64
CH = 1024
KW = 31
WINDOW = 128


EPS = 1e-06
LAST_FROM = 1
ROWS_BY = 2


def passed_along(value, axis, steps):
    count = lax.axis_size(axis)
    leading, last = (max(0, -steps), min(count, count - steps))
    return lax.ppermute(value, axis, [(source, source + steps) for source in range(leading, last)])


def row_norm(inputs, scale_vec):
    squares = jnp.mean(inputs * inputs, axis=-1, keepdims=True)
    return inputs * lax.rsqrt(squares + EPS) * scale_vec


def whole_features(tokens):
    if lax.axis_size("tp") != 2:
        return lax.all_gather(tokens, "tp", axis=1, tiled=True)
    other = lax.ppermute(tokens, "tp", [(0, 1), (1, 0)])
    first = lax.axis_index("tp") == 0
    return jnp.concatenate(
        [jnp.where(first, tokens, other), jnp.where(first, other, tokens)], 1
    )


def exchanged(value, axis, bit):
    count = lax.axis_size(axis)
    return lax.ppermute(value, axis, [(source, source ^ bit) for source in range(count)])


def after(value, others):
    return lax.optimization_barrier((value, *others))[0]


def reordered(value, axis, order, dim):
    count = lax.axis_size(axis)
    place = lax.axis_index(axis)
    width = value.shape[dim] // count
    blocks = [0]
    for bit in order:
        blocks = blocks + [block ^ bit for block in blocks]
    return jnp.concatenate(
        [
            lax.dynamic_slice_in_dim(value, (place ^ block) * width, width, dim)
            for block in blocks
        ],
        dim,
    )


def orders_of(count):
    bits = []
    while 2 ** len(bits) < count:
        bits.append(2 ** len(bits))
    if len(bits) != 4 or 2 ** len(bits) != count:
        return None
    one, two, four, eight = bits
    return (eight, two, four, one), (eight, four, one, two), (one, eight, two, four)


def gathered_products(normed, groups, last):
    orders = orders_of(lax.axis_size("sp"))
    packed = [jnp.concatenate(group, 1) for group in groups]
    last = jnp.concatenate(last, 1)
    if orders is None:
        packed = [lax.all_gather(part, "sp", axis=0, tiled=True) for part in packed]
        rows = [normed] * len(packed)
    else:
        rows = [reordered(normed, "sp", order, 1) for order in orders]
        for step in range(len(orders[0])):
            if step == LAST_FROM:
                last = after(last, packed)
            if step == ROWS_BY:
                tied = lax.optimization_barrier((*packed, *rows))
                packed, rows = list(tied[: len(packed)]), list(tied[len(packed) :])
            packed = [
                jnp.concatenate([part, exchanged(part, "sp", order[step])], 0)
                for part, order in zip(packed, orders)
            ]
    last = lax.all_gather(last, "sp", axis=0, tiled=True)
    products = []
    for group, part, inputs in zip(groups, packed, rows):
        start = 0
        for weight in group:
            columns = part[:, start : start + weight.shape[1]]
            products.append(jnp.dot(inputs, columns, preferred_element_type=jnp.float32))
            start += weight.shape[1]
    return products, last


def sum_scattered(features, back):
    contract = (((1,), (1,)), ((), ()))

    def product(rows):
        result = lax.dot_general(rows, back, contract, preferred_element_type=jnp.float32)
        return result.astype(jnp.bfloat16)

    if lax.axis_size("tp") != 2:
        return lax.psum_scatter(product(features), "tp", scatter_dimension=0, tiled=True)
    half = features.shape[0] // 2
    core = lax.axis_index("tp")
    theirs = product(lax.dynamic_slice_in_dim(features, (1 - core) * half, half, 0))
    came = exchanged(theirs, "tp", 1)
    ours = product(lax.dynamic_slice_in_dim(features, core * half, half, 0))
    return (ours.astype(jnp.float32) + came.astype(jnp.float32)).astype(jnp.bfloat16)


def local(
    tokens,
    norm_gain,
    w_query,
    w_key,
    w_value,
    w_glu_a,
    w_glu_b,
    q_gain,
    k_gain,
    sink_logit,
    conv_taps,
    chan_gain,
    chan_bias,
    w_attn_back,
    w_conv_back,
):
    row_count = tokens.shape[0]
    q_local = w_query.shape[1] // HEAD
    kv_local = w_key.shape[1] // HEAD
    group_size = q_local // kv_local
    kv_width = kv_local * HEAD
    gathered = whole_features(tokens)
    normed = row_norm(gathered.astype(jnp.float32), norm_gain).astype(jnp.bfloat16)
    products, back = gathered_products(
        normed, ((w_query, w_key), (w_glu_a, w_value), (w_glu_b,)), (w_attn_back, w_conv_back)
    )
    query_raw, key_raw, glu_a, value_raw, glu_b = products
    queries = row_norm(query_raw.reshape(row_count, q_local, HEAD), q_gain).astype(jnp.bfloat16)
    key_rows = (
        row_norm(key_raw.reshape(row_count, kv_local, HEAD), k_gain)
        .astype(jnp.bfloat16)
        .reshape(row_count, kv_width)
    )
    value_rows = value_raw.astype(jnp.bfloat16)
    gated_rows = (glu_a * jax.nn.sigmoid(glu_b)).astype(jnp.bfloat16)
    key_value = jnp.concatenate([key_rows, value_rows], 1)
    key_value_rim = passed_along(key_value[row_count - WINDOW :], "sp", 1)
    gated_rim = passed_along(gated_rows[row_count - (KW - 1) :], "sp", 1)
    block_count = row_count // WINDOW
    extended = jnp.concatenate([key_value_rim, key_value], 0).reshape(
        block_count + 1, WINDOW, 2 * kv_width
    )
    band = jnp.concatenate([extended[:-1], extended[1:]], 1)
    key_band = band[:, :, :kv_width].reshape(block_count, 2 * WINDOW, kv_local, HEAD)
    value_band = band[:, :, kv_width:].reshape(block_count, 2 * WINDOW, kv_local, HEAD)
    grouped = queries.reshape(block_count, WINDOW, kv_local, group_size, HEAD)
    scores = jnp.einsum(
        "nqhgd,nkhd->nhgqk", grouped, key_band, preferred_element_type=jnp.float32
    ) * HEAD ** (-0.5)
    offsets = jnp.arange(WINDOW, dtype=jnp.int32)
    band_offsets = jnp.arange(2 * WINDOW, dtype=jnp.int32)
    distance = WINDOW + offsets[:, None] - band_offsets[None, :]
    allowed = (distance >= 0) & (distance < WINDOW)
    anchor = lax.axis_index("sp") * row_count
    key_position = (
        anchor
        + jnp.arange(block_count, dtype=jnp.int32)[:, None] * WINDOW
        - WINDOW
        + band_offsets[None, :]
    )
    visible = (allowed[None, :, :] & (key_position[:, None, :] >= 0))[:, None, None]
    sink_table = sink_logit.reshape(kv_local, group_size)[None, :, :, None, None]
    masked = jnp.where(visible, scores, -jnp.inf)
    largest = jnp.maximum(jnp.max(masked, axis=-1, keepdims=True), sink_table)
    weights = jnp.where(visible, jnp.exp(scores - largest), 0.0)
    weight_sum = jnp.sum(weights, axis=-1, keepdims=True) + jnp.exp(sink_table - largest)
    log_weight = (largest + jnp.log(weight_sum))[..., 0]
    log_weight = jnp.transpose(log_weight, (1, 2, 0, 3)).reshape(q_local, row_count)
    probabilities = (weights / weight_sum).astype(jnp.bfloat16)
    attended = jnp.einsum(
        "nhgqk,nkhd->nqhgd", probabilities, value_band, preferred_element_type=jnp.float32
    )
    attended = attended.astype(jnp.bfloat16).reshape(row_count, q_local * HEAD)
    gate_extended = jnp.concatenate([gated_rim, gated_rows], 0).astype(jnp.float32)
    convolved = jnp.zeros((row_count, gated_rows.shape[1]), jnp.float32)
    for tap_index in range(KW):
        convolved = (
            convolved + conv_taps[tap_index] * gate_extended[tap_index : tap_index + row_count]
        )
    channel_sums = lax.psum(
        (jnp.sum(convolved, axis=1), jnp.sum(convolved * convolved, axis=1)), "tp"
    )
    center = (channel_sums[0] / CH)[:, None]
    spread = (channel_sums[1] / CH)[:, None] - center * center
    conv_rows = jax.nn.silu(
        (convolved - center) * lax.rsqrt(spread + EPS) * chan_gain + chan_bias
    ).astype(jnp.bfloat16)
    features = jnp.concatenate([attended, conv_rows], 1)
    summed = sum_scattered(features, back)
    return (summed, log_weight)


def solution(mesh):
    placed = (
        P("sp", "tp"),
        P(),
        P("sp", "tp"),
        P("sp", "tp"),
        P("sp", "tp"),
        P("sp", "tp"),
        P("sp", "tp"),
        P(),
        P(),
        P("tp"),
        P(None, "tp"),
        P("tp"),
        P("tp"),
        P("sp", "tp"),
        P("sp", "tp"),
    )
    return jax.shard_map(
        local,
        mesh=mesh,
        in_specs=placed,
        out_specs=(P(("sp", "tp"), None), P("tp", "sp")),
        check_vma=False,
    )
```
